32 devices in a mesh: ep: 8 (over z, core), tp: 4 (over y, x).
Axes of the slice: x: 2, y: 2, z: 4, core: 2. Of those that a mesh axis runs over, the one named last changes fastest.
Arguments:
- q_latent: bfloat16 [1536, 512], P('ep'), may hold values from -6 to 6
- kv_latent: bfloat16 [1536, 256], P('ep'), may hold values from -6 to 6
- rope_key: bfloat16 [1536, 64], P('ep'), may hold values from -900 to 900
- q_gain: float32 [512], replicated, may hold values from 0.1 to 1.9
- kv_gain: float32 [256], replicated, may hold values from 0.1 to 1.9
- w_query: bfloat16 [512, 3072], P(None, 'tp'), may hold values from -0.25 to 0.25
- w_key: bfloat16 [256, 2048], P(None, 'tp'), may hold values from -0.375 to 0.375
- w_value: bfloat16 [256, 2048], P(None, 'tp'), may hold values from -0.375 to 0.375
- w_mix_out: bfloat16 [2048, 2048], P('tp'), may hold values from -0.125 to 0.125
- expert_in: bfloat16 [1024, 2048], P('ep'), may hold values from -6 to 6
- norm_gain: float32 [2048], replicated, may hold values from 0.1 to 1.9
- routes: int32 [1024, 2], P('ep'), may hold values from 0 to 7, all different within a row; in each aligned block of 128 rows (0 to 127, 128 to 255, ...) at most 64 rows name the same one
- route_scores: float32 [1024, 2], P('ep'), may hold values from 0.05 to 1
- w_gate: bfloat16 [8, 2048, 4096], P('ep', None, 'tp'), may hold values from -0.125 to 0.125
- w_up: bfloat16 [8, 2048, 4096], P('ep', None, 'tp'), may hold values from -0.125 to 0.125
- w_down: bfloat16 [8, 4096, 2048], P('ep', 'tp'), may hold values from -0.125 to 0.125
Outputs:
- mixed: bfloat16 [1536, 2048], P(('ep', 'tp'))
- expert_out: bfloat16 [1024, 2048], P('ep', 'tp')
The draws below stay inside these ranges and needn't reach their ends.
Inputs may be any that keep to these rules, and one draw needn't show every extreme that they name: `routes`: each row names 2 different experts; in the rows of one index of ep no expert is named by more than 64 rows, a bound that some block reaches.
All inputs are finite; a program needn't handle non-finite values.
Results may differ from the reference program's by a relative error of at most 0.03.
The reference program's roundings to bfloat16 on the way count: a program that leaves them out, or rounds other values in their place, can miss the bound.
Values may be sent and summed in bfloat16 or wider, within the bound.
No kernel may reach another device: no remote copies, remote signals or barrier semaphores. Data moves between devices by JAX's collectives and lax.ppermute only.
A program may use at most 64 MiB of HBM per device.

```python
import math
import jax
import jax.numpy as jnp
import numpy as np
from jax import lax

D = 2048
HEADS = 16
QR = 512
KVR = 256
NOPE = 128
ROPE = 64
VDIM = 128
FF = 4096
TOP = 2
TOKA = 192
TOKB = 128
EXPERTS = 8
CAP = 64
N_EP = 8
N_TP = 4


def draw_rope_key(key, part):
    length = TOKA * N_EP
    base = jnp.clip(jax.random.normal(jax.random.fold_in(key, 11), (length, ROPE), jnp.float32), -6.0, 6.0)
    return base.astype(jnp.bfloat16)


def strengthened(array, rng, source, target, shards_of, factor):
    def block_of(axis_at):
        return (jnp.arange(array.shape[axis_at]) // (array.shape[axis_at] // shards_of)).reshape((-1,) + (1,) * (array.ndim - 1 - axis_at))

    first = jax.random.permutation(rng, shards_of)[block_of(target)]
    far = (block_of(target) + shards_of // 2) % shards_of
    return jnp.where((block_of(source) == first) | (block_of(source) == far), factor * array, array)


def level_of(key, extent, cuts, least, top_value):
    level, own = 1.0, jax.random.fold_in(key, 6)
    for axis_at, shards_of in cuts:
        heights = jnp.exp(jax.random.uniform(jax.random.fold_in(own, axis_at), (shards_of,), jnp.float32, least / len(cuts), top_value / len(cuts)))
        level = level * jnp.repeat(heights, extent[axis_at] // shards_of).reshape([-1 if axis == axis_at else 1 for axis in range(len(extent))])
    return level


def assign_block(key, own, number, rows, count, top, bound, skew):
    ranking = jax.random.permutation(key, count)
    heavy_load, usual = load_shares(count, rows * top, bound, skew, True), load_shares(count, rows * top, bound, skew, False)
    places = jnp.arange(count)

    def named(tallies, offset_by):
        used = int((tallies > 0).sum())
        fixed = max(1, used // 4)
        moved = fixed + (places - fixed + offset_by * (used - fixed)) % max(1, count - fixed)
        return jnp.zeros((count,), jnp.int32).at[ranking[jnp.where(places < fixed, places, moved)]].set(jnp.asarray(tallies, jnp.int32))

    tallies = jnp.where(number % 4 == 0, named(heavy_load, number // 4), named(usual, number - number // 4 - 1))
    mixed = jax.random.permutation(jax.random.fold_in(own, 3), count)
    source_of, taker = mixed[0:count // 2 * 2:2], mixed[1:count // 2 * 2:2]
    room = jnp.minimum(tallies[source_of] - 1, bound - tallies[taker]) // 2
    room = jnp.where((source_of == ranking[0]) | (taker == ranking[0]) | (tallies[taker] == 0), 0, jnp.maximum(room, 0))
    moved = jax.random.randint(jax.random.fold_in(own, 4), (count // 2,), 0, 1 << 20) % (room + 1)
    tallies = tallies.at[source_of].add(-moved).at[taker].add(moved)
    labels = jnp.searchsorted(jnp.cumsum(tallies), jnp.arange(rows * top), side="right").astype(jnp.int32)
    listing = labels.reshape(top, rows).T
    listing = listing[jax.random.permutation(jax.random.fold_in(own, 1), rows)]
    offset_by = jax.random.randint(jax.random.fold_in(own, 2), (rows, 1), 0, top)
    return jnp.take_along_axis(listing, (jnp.arange(top)[None, :] + offset_by) % top, axis=1)


def load_shares(amount, total, limit, lean, full):
    portions = [(1 << 20) // math.isqrt(grade ** lean) + 1 for grade in range(1, amount + 1)]
    largest = limit if full else min(limit, max(-(-total // amount), total * portions[0] // sum(portions)))
    least = 1 if total - largest >= amount - 1 else 0
    counts, surplus = [largest] + [least] * (amount - 1), total - largest - least * (amount - 1)
    while surplus > 0:
        movable = [i for i in range(1, amount) if counts[i] < largest] or [i for i in range(1, amount) if counts[i] < limit]
        pool, budget = sum([portions[i] for i in movable]), surplus
        for i in movable:
            addition = min(limit - counts[i], max(1, budget * portions[i] // pool), surplus)
            counts[i] = counts[i] + addition
            surplus = surplus - addition
    return np.array(counts)


def gaussian(own_key, dims, scale, limit, shards=(), held_as=jnp.bfloat16):
    entries = jax.random.normal(own_key, dims, jnp.float32) * scale
    if len(shards) > 0:
        entries = level_of(own_key, dims, shards, -0.22, 0.18) * entries
    return jnp.clip(entries, min=-limit, max=limit).astype(held_as)


def heavy_noise(key, shape, width, most, shards, heavy, kind=jnp.bfloat16):
    result = width * jax.random.normal(key, shape, jnp.float32)
    if shards:
        result = result * level_of(key, shape, shards, -0.22, 0.18)
    return jnp.clip(strengthened(result, jax.random.fold_in(key, 3), *heavy), -most, most).astype(kind)


def setup_inputs(seed: int = 0) -> dict:
    splits = jax.random.split(jax.random.key(seed), 17)
    q_latent = gaussian(splits[0], (TOKA * N_EP, QR), 1.0, 6.0, ((0, 8),))
    kv_latent = gaussian(splits[1], (TOKA * N_EP, KVR), 1.0, 6.0, ((0, 8),))
    rope_key = draw_rope_key(jax.random.fold_in(splits[16], 71), 0)
    q_gain = jnp.clip(1.0 + 0.18 * jax.random.normal(splits[3], (QR,), jnp.float32), 0.1, 1.9)
    kv_gain = jnp.clip(1.0 + 0.18 * jax.random.normal(splits[4], (KVR,), jnp.float32), 0.1, 1.9)
    w_query = gaussian(splits[5], (QR, HEADS * (NOPE + ROPE)), QR ** -0.5, 0.25, ((1, 4),))
    w_key = gaussian(splits[6], (KVR, HEADS * NOPE), KVR ** -0.5, 0.375, ((1, 4),))
    w_value = gaussian(splits[7], (KVR, HEADS * VDIM), KVR ** -0.5, 0.375, ((1, 4),))
    w_mix_out = gaussian(splits[8], (HEADS * VDIM, D), (HEADS * VDIM) ** -0.5, 0.125, ((0, 4),))
    expert_in = gaussian(splits[9], (TOKB * N_EP, D), 1.0, 6.0, ((0, 8),))
    norm_gain = jnp.clip(1.0 + 0.18 * jax.random.normal(splits[10], (D,), jnp.float32), 0.1, 1.9)
    routes_keys = jax.random.split(jax.random.fold_in(splits[11], 1), (TOKB * N_EP) // TOKB)
    routes_turns = jax.random.permutation(jax.random.fold_in(splits[11], 3), (TOKB * N_EP) // TOKB)
    routes = jax.vmap(lambda own, number: assign_block(jax.random.fold_in(splits[11], 2), own, number, TOKB, EXPERTS, TOP, CAP, 2))(routes_keys, routes_turns).reshape((TOKB * N_EP, TOP))
    route_scores = jnp.clip(jnp.exp(math.log(1.0) - 2.9957323 * jax.random.uniform(splits[12], (TOKB * N_EP, TOP), jnp.float32) ** level_of(splits[12], (TOKB * N_EP, TOP), ((0, 8),), -0.2, 0.2)), 0.05, 1.0)
    w_gate = gaussian(splits[13], (EXPERTS, D, FF), D ** -0.5, 0.125, ((0, 8), (2, 4)))
    w_up = gaussian(splits[14], (EXPERTS, D, FF), D ** -0.5, 0.125, ((0, 8), (2, 4)))
    w_down = heavy_noise(splits[15], (EXPERTS, FF, D), FF ** -0.5, 0.125, ((0, 8), (1, 4)), (1, 2, 4, 2.0))
    return {"q_latent": q_latent, "kv_latent": kv_latent, "rope_key": rope_key, "q_gain": q_gain, "kv_gain": kv_gain, "w_query": w_query, "w_key": w_key, "w_value": w_value, "w_mix_out": w_mix_out, "expert_in": expert_in, "norm_gain": norm_gain, "routes": routes, "route_scores": route_scores, "w_gate": w_gate, "w_up": w_up, "w_down": w_down}


eps_norm = 1e-05
rope_base = 10000.0

def rms_scale(values, gain):
    wide = values.astype(jnp.float32)
    return wide * lax.rsqrt(lax.optimization_barrier(jnp.mean(wide * wide, -1, keepdims=True)) + eps_norm) * gain

def rotate(values, cosine, sine):
    first, second = jnp.split(values, 2, axis=-1)
    return jnp.concatenate([first * cosine - second * sine, first * sine + second * cosine], -1)

def angles(positions):
    inverse = rope_base ** (-jnp.arange(0, ROPE, 2).astype(jnp.float32) / ROPE)
    phase = positions[:, None] * inverse[None, :]
    return (jnp.cos(phase), jnp.sin(phase))

def grouped_sum(left, right, groups):
    length = left.shape[0]
    inner = left.shape[1] // groups
    left_groups = jnp.transpose(left.reshape(length, groups, inner), (1, 0, 2))
    right_groups = right.reshape(groups, inner, right.shape[1])

    def add_group(total, pair):
        part = jnp.dot(pair[0], pair[1], preferred_element_type=jnp.float32).astype(jnp.bfloat16)
        part = lax.optimization_barrier(part)
        return (total + part.astype(jnp.float32), None)
    start_total = jnp.zeros((length, right.shape[1]), jnp.float32)
    total, unused = lax.scan(add_group, start_total, (left_groups, right_groups))
    return total.astype(jnp.bfloat16)

def reference(q_latent, kv_latent, rope_key, q_gain, kv_gain, w_query, w_key, w_value, w_mix_out, expert_in, norm_gain, routes, route_scores, w_gate, w_up, w_down):
    length = q_latent.shape[0]
    positions = jnp.arange(length, dtype=jnp.int32).astype(jnp.float32)
    cosine, sine = angles(positions)
    q_normed = rms_scale(q_latent, q_gain).astype(jnp.bfloat16)
    kv_normed = rms_scale(kv_latent, kv_gain).astype(jnp.bfloat16)
    query = jnp.dot(q_normed, w_query, preferred_element_type=jnp.float32).astype(jnp.bfloat16)
    query = query.reshape(length, HEADS, NOPE + ROPE)
    q_pass = query[:, :, :NOPE]
    q_rot = rotate(query[:, :, NOPE:].astype(jnp.float32), cosine[:, None, :], sine[:, None, :]).astype(jnp.bfloat16)
    k_rot = rotate(rope_key.astype(jnp.float32), cosine, sine).astype(jnp.bfloat16)
    keys = jnp.dot(kv_normed, w_key, preferred_element_type=jnp.float32).astype(jnp.bfloat16).reshape(length, HEADS, NOPE)
    values = jnp.dot(kv_normed, w_value, preferred_element_type=jnp.float32).astype(jnp.bfloat16).reshape(length, HEADS, VDIM)
    factor = (NOPE + ROPE) ** (-0.5)

    def attend_head(inputs):
        pass_head, rot_head, key_head, value_head = inputs
        scores = jnp.dot(pass_head, key_head.T, preferred_element_type=jnp.float32)
        scores = (scores + jnp.dot(rot_head, k_rot.T, preferred_element_type=jnp.float32)) * factor
        peak = lax.optimization_barrier(jnp.max(scores, -1, keepdims=True))
        weights = jnp.exp(scores - peak)
        total = lax.optimization_barrier(jnp.sum(weights, -1, keepdims=True))
        summed = jnp.dot(weights.astype(jnp.bfloat16), value_head, preferred_element_type=jnp.float32)
        return (summed / total).astype(jnp.bfloat16)
    per_head = lax.map(attend_head, (jnp.transpose(q_pass, (1, 0, 2)), jnp.transpose(q_rot, (1, 0, 2)), jnp.transpose(keys, (1, 0, 2)), jnp.transpose(values, (1, 0, 2))))
    attended = jnp.transpose(per_head, (1, 0, 2)).reshape(length, HEADS * VDIM)
    mixed = grouped_sum(attended, w_mix_out, N_TP)
    token_total = expert_in.shape[0]
    wide = expert_in.astype(jnp.float32)
    centered = wide - lax.optimization_barrier(jnp.mean(wide, -1, keepdims=True))
    normed = (centered * lax.rsqrt(lax.optimization_barrier(jnp.mean(centered * centered, -1, keepdims=True)) + eps_norm) * norm_gain).astype(jnp.bfloat16)
    shares = route_scores / lax.optimization_barrier(jnp.sum(route_scores, -1, keepdims=True))
    flat_expert = routes.reshape(-1).astype(jnp.int32)
    copies = flat_expert.shape[0]
    group_of = (jnp.arange(copies, dtype=jnp.int32) // (TOKB * TOP)).astype(jnp.int32)
    onehot = (flat_expert[:, None] == jnp.arange(EXPERTS, dtype=jnp.int32)[None, :]).astype(jnp.int32)
    within = onehot.reshape(N_EP, TOKB * TOP, EXPERTS)
    before = (jnp.cumsum(within, 1) - within).reshape(copies, EXPERTS)
    rank = lax.optimization_barrier(jnp.sum(before * onehot, 1)).astype(jnp.int32)
    slot = (group_of * CAP + rank).astype(jnp.int32)
    source = (jnp.arange(copies, dtype=jnp.int32) // TOP).astype(jnp.int32)
    table = jnp.full((EXPERTS, N_EP * CAP), token_total, jnp.int32).at[flat_expert, slot].set(source)
    padded = jnp.concatenate([normed, jnp.zeros((1, D), jnp.bfloat16)], 0)

    def one_expert(inputs):
        index, gate_weight, up_weight, down_weight = inputs
        arrived = padded[index]
        gate = jnp.dot(arrived, gate_weight, preferred_element_type=jnp.float32)
        up = jnp.dot(arrived, up_weight, preferred_element_type=jnp.float32)
        hidden = (jax.nn.silu(gate) * up).astype(jnp.bfloat16)
        return grouped_sum(hidden, down_weight, N_TP)
    results = lax.map(one_expert, (table, w_gate, w_up, w_down))
    picked = results[flat_expert, slot].astype(jnp.float32).reshape(token_total, TOP, D)
    expert_out = lax.optimization_barrier(jnp.sum(picked * shares[:, :, None], 1)).astype(jnp.bfloat16)
    return (mixed, expert_out)
```

```python
import jax
import jax.numpy as jnp
from jax import lax
from jax.sharding import PartitionSpec as P

NOPE = 128
ROPE = 64
VDIM = 128


eps_norm = 1e-05
rope_base = 10000.0


def rms_scale(values, gain):
    wide = values.astype(jnp.float32)
    return wide * lax.rsqrt(jnp.mean(wide * wide, -1, keepdims=True) + eps_norm) * gain


def rotate(values, cosine, sine):
    first, second = jnp.split(values, 2, axis=-1)
    return jnp.concatenate([first * cosine - second * sine, first * sine + second * cosine], -1)


def angles(positions):
    inverse = rope_base ** (-jnp.arange(0, ROPE, 2).astype(jnp.float32) / ROPE)
    phase = positions[:, None] * inverse[None, :]
    return (jnp.cos(phase), jnp.sin(phase))


def tp_bits():
    return (lax.axis_size("tp") - 1).bit_length()


def swap(value, axis, flip):
    pairs = [(i, i ^ flip) for i in range(lax.axis_size(axis))]
    return lax.ppermute(value, axis, pairs)


def gather_tp(value, order):
    held = {0: value}
    for bit in order:
        held.update({j ^ (1 << bit): swap(v, "tp", 1 << bit) for j, v in list(held.items())})
    return held


def reduce_tp(blocks, order):
    held = dict(blocks)
    for bit in order:
        flip = 1 << bit
        sent = {j: swap(v, "tp", flip) for j, v in held.items() if j & flip}
        held = {
            j: (v.astype(jnp.float32) + sent[j ^ flip].astype(jnp.float32)).astype(jnp.bfloat16)
            for j, v in held.items()
            if not j & flip
        }
    return held[0]


def pick(blocks, index):
    return lax.dynamic_index_in_dim(blocks, index, 0, keepdims=False)


def gather_latent(packed):
    size = lax.axis_size("ep")
    mine = [packed] + [swap(packed, "ep", k) for k in range(2, size, 2)]
    mine = jnp.concatenate(mine, 0)
    return jnp.concatenate([mine, swap(mine, "ep", 1)], 0)


def mixer(q_latent, kv_latent, rope_key, q_gain, kv_gain, w_query, w_key, w_value, w_mix_out):
    token_count = q_latent.shape[0]
    head_count = w_key.shape[1] // NOPE
    rank = kv_latent.shape[1]
    offset = lax.axis_index("ep") * token_count
    positions = (offset + jnp.arange(token_count, dtype=jnp.int32)).astype(jnp.float32)
    cosine, sine = angles(positions)
    kv_normed = rms_scale(kv_latent, kv_gain).astype(jnp.bfloat16)
    key_turned = rotate(rope_key.astype(jnp.float32), cosine, sine).astype(jnp.bfloat16)
    gathered = gather_latent(jnp.concatenate([kv_normed, key_turned], 1))
    latent = gathered[:, :rank]
    turned = gathered[:, rank:]
    q_normed = rms_scale(q_latent, q_gain).astype(jnp.bfloat16)
    query = jnp.dot(q_normed, w_query, preferred_element_type=jnp.float32).astype(jnp.bfloat16)
    query = query.reshape(token_count, head_count, NOPE + ROPE)
    q_pass = query[:, :, :NOPE]
    q_turned = rotate(
        query[:, :, NOPE:].astype(jnp.float32), cosine[:, None, :], sine[:, None, :]
    ).astype(jnp.bfloat16)
    factor = (NOPE + ROPE) ** (-0.5)
    count = latent.shape[0]
    keys = jnp.dot(latent, w_key, preferred_element_type=jnp.float32).astype(jnp.bfloat16)
    keys = keys.reshape(count, head_count, NOPE)
    values = jnp.dot(latent, w_value, preferred_element_type=jnp.float32).astype(jnp.bfloat16)
    values = values.reshape(count, head_count, VDIM)
    scores = jnp.einsum("qhd,khd->hqk", q_pass, keys, preferred_element_type=jnp.float32)
    scores = (
        scores + jnp.einsum("qhd,kd->hqk", q_turned, turned, preferred_element_type=jnp.float32)
    ) * factor
    weights = jnp.exp(scores - jnp.max(scores, -1)[:, :, None])
    total = jnp.sum(weights, -1)
    summed = jnp.einsum(
        "hqk,khd->qhd", weights.astype(jnp.bfloat16), values, preferred_element_type=jnp.float32
    )
    attended = (summed / jnp.transpose(total)[:, :, None]).astype(jnp.bfloat16)
    attended = attended.reshape(token_count, head_count * VDIM)
    return jnp.dot(attended, w_mix_out, preferred_element_type=jnp.float32).astype(jnp.bfloat16)


def mix_sum(part):
    size = lax.axis_size("tp")
    own = lax.axis_index("tp")
    rows, width = part.shape
    blocks = part.reshape(size, rows // size, width)
    own_blocks = {j: pick(blocks, own ^ j) for j in range(size)}
    order = list(range(tp_bits()))
    half = width // 2
    low = reduce_tp({j: v[:, :half] for j, v in own_blocks.items()}, order)
    high = reduce_tp({j: v[:, half:] for j, v in own_blocks.items()}, order[::-1])
    return jnp.concatenate([low, high], 1)


def dispatch(expert_in, norm_gain, routes):
    token_count, width = expert_in.shape
    choose = routes.shape[1]
    expert_count = lax.axis_size("ep")
    size = lax.axis_size("tp")
    slots = 2 * choose * token_count // expert_count
    wide = expert_in.astype(jnp.float32)
    centered = wide - jnp.mean(wide, -1, keepdims=True)
    scale = lax.rsqrt(jnp.mean(centered * centered, -1, keepdims=True) + eps_norm)
    part = width // size
    start = lax.axis_index("tp") * part
    normed = (
        lax.dynamic_slice_in_dim(centered, start, part, 1)
        * scale
        * lax.dynamic_slice_in_dim(norm_gain, start, part, 0)
    ).astype(jnp.bfloat16)
    relative = routes ^ lax.axis_index("ep")
    onehot = relative[:, :, None] == jnp.arange(expert_count, dtype=jnp.int32)
    named = jnp.sum(onehot.astype(jnp.float32), 1).astype(jnp.bfloat16)
    lane = jnp.arange(token_count, dtype=jnp.int32)
    earlier = (lane[None, :] < lane[:, None]).astype(jnp.bfloat16)
    before = jnp.dot(earlier, named, preferred_element_type=jnp.float32)
    rank = jnp.sum(jnp.where(onehot, before[:, None, :], 0.0), -1).astype(jnp.int32)
    target = relative * slots + rank
    chosen = jnp.arange(expert_count * slots, dtype=jnp.int32)[:, None]
    table = sum((chosen == target[:, k][None, :]).astype(jnp.bfloat16) for k in range(choose))
    outgoing = jnp.dot(table, normed, preferred_element_type=jnp.float32).astype(jnp.bfloat16)
    outgoing = outgoing.reshape(expert_count, slots, part)
    arrived = [outgoing[0]] + [swap(outgoing[k], "ep", k) for k in range(1, expert_count)]
    return arrived, target, slots


def assemble(arrived):
    size = lax.axis_size("tp")
    own = lax.axis_index("tp")
    order = list(range(tp_bits()))
    half = len(arrived) // 2
    rows = []
    for piece, way in ((arrived[:half], order), (arrived[half:], order[::-1])):
        held = gather_tp(jnp.concatenate(piece, 0), way)
        stacked = jnp.stack([held[j] for j in range(size)], 0)
        rows.append(jnp.concatenate([pick(stacked, own ^ i) for i in range(size)], 1))
    return jnp.concatenate(rows, 0)


def apply_expert(rows, w_gate, w_up, w_down):
    gate = jnp.dot(rows, w_gate[0], preferred_element_type=jnp.float32)
    up = jnp.dot(rows, w_up[0], preferred_element_type=jnp.float32)
    hidden = (jax.nn.silu(gate) * up).astype(jnp.bfloat16)
    size = lax.axis_size("tp")
    own = lax.axis_index("tp")
    order = list(range(tp_bits()))
    half = rows.shape[0] // 2
    sums = []
    for piece, way in ((hidden[half:], order), (hidden[:half], order[::-1])):
        part = jnp.dot(piece, w_down[0], preferred_element_type=jnp.float32)
        part = part.astype(jnp.bfloat16)
        span = part.shape[1] // size
        blocks = {
            j: lax.dynamic_slice_in_dim(part, (own ^ j) * span, span, 1) for j in range(size)
        }
        sums.append(reduce_tp(blocks, way))
    return sums[::-1]


def send_back(sums, slots):
    count = lax.axis_size("ep")
    half = count // 2
    pieces = []
    for k in range(count):
        start = (k % half) * slots
        value = sums[k // half][start : start + slots]
        pieces.append(swap(value, "ep", k) if k else value)
    return jnp.concatenate(pieces, 0)


def combine(returned, target, route_scores):
    shares = route_scores / jnp.sum(route_scores, -1, keepdims=True)
    picked = returned[target.reshape(-1)].reshape(target.shape + (returned.shape[1],))
    return jnp.sum(picked.astype(jnp.float32) * shares[:, :, None], 1).astype(jnp.bfloat16)


def body(
    q_latent,
    kv_latent,
    rope_key,
    q_gain,
    kv_gain,
    w_query,
    w_key,
    w_value,
    w_mix_out,
    expert_in,
    norm_gain,
    routes,
    route_scores,
    w_gate,
    w_up,
    w_down,
):
    arrived, target, slots = dispatch(expert_in, norm_gain, routes)
    part = mixer(
        q_latent, kv_latent, rope_key, q_gain, kv_gain, w_query, w_key, w_value, w_mix_out
    )
    rows, part = lax.optimization_barrier((assemble(arrived), part))
    mixed = mix_sum(part)
    sums = apply_expert(rows, w_gate, w_up, w_down)
    expert_out = combine(send_back(sums, slots), target, route_scores)
    return (mixed, expert_out)


def solution(mesh):
    in_specs = (
        P("ep", None),
        P("ep", None),
        P("ep", None),
        P(),
        P(),
        P(None, "tp"),
        P(None, "tp"),
        P(None, "tp"),
        P("tp", None),
        P("ep", None),
        P(),
        P("ep", None),
        P("ep", None),
        P("ep", None, "tp"),
        P("ep", None, "tp"),
        P("ep", "tp", None),
    )
    out_specs = (P(("ep", "tp"), None), P("ep", "tp"))
    return jax.shard_map(body, mesh=mesh, in_specs=in_specs, out_specs=out_specs, check_vma=False)
```
